256 devices in a mesh: sp: 64 (over z, x, core), tp: 4 (over y).
Axes of the slice: x: 4, y: 4, z: 8, core: 2. Of those that a mesh axis runs over, the one named last changes fastest.
Arguments:
- resid: bfloat16 [16384, 4096], P('sp'), may hold values from -6 to 6
- pool_in: bfloat16 [16384, 1024], P('sp', 'tp'), may hold values from -6 to 6
- pool_mix: bfloat16 [4, 256, 256], P('tp'), may hold values from -0.375 to 0.375
- pool_gain: float32 [1024], P('tp'), may hold values from 0.1 to 1.9
- out_proj: bfloat16 [1024, 4096], P('tp'), may hold values from -0.1875 to 0.1875
- norm_gain: float32 [4096], replicated, may hold values from 0.1 to 1.9
- w_gate: bfloat16 [64, 4096, 1024], P('sp', None, 'tp'), may hold values from -0.09375 to 0.09375
- w_up: bfloat16 [64, 4096, 1024], P('sp', None, 'tp'), may hold values from -0.09375 to 0.09375
- w_down: bfloat16 [64, 1024, 4096], P('sp', 'tp'), may hold values from -0.1875 to 0.1875
- routes: int32 [16384, 2], P('sp'), may hold values from 0 to 63, all different within a row; in each aligned block of 64 rows (0 to 63, 64 to 127, ...) at most 4 rows name the same one
- route_weight: float32 [16384, 2], P('sp'), may hold values from 0.25 to 2.5
Outputs:
- layer_out: bfloat16 [16384, 4096], P(('sp', 'tp'))
The draws below stay inside these ranges and needn't reach their ends.
Inputs may be any that keep to these rules, and one draw needn't show every extreme that they name: `routes`: in each aligned block of 64 tokens no expert is named by more than 4 of the block's rows, and the two experts of a token differ.
All inputs are finite; a program needn't handle non-finite values.
Results may differ from the reference program's by a relative error of at most 0.015.
Values may be sent and summed in bfloat16 or wider, within the bound.
No kernel may reach another device: no remote copies, remote signals or barrier semaphores. Data moves between devices by JAX's collectives and lax.ppermute only.
A program may use at most 128 MiB of HBM per device.

```python
import math
import jax
import jax.numpy as jnp
import numpy as np
from jax import lax

D = 4096
GROUPS = 4
PCH = 256
POOLW = 1024
FF = 1024
FF_PART = 256
TOP = 2
TOK_SUB = 64
TOKENS = 16384
EXPERTS = 64
CAP = 4
N_TP = 4


def levels(key, extent, pieces, smallest, top_value):
    def one(axis_at, blocks):
        steps = jax.random.uniform(jax.random.fold_in(jax.random.fold_in(key, 6), axis_at), (blocks,), jnp.float32, smallest / len(pieces), top_value / len(pieces))
        return jnp.repeat(jnp.exp(steps), extent[axis_at] // blocks).reshape((-1,) + (1,) * (len(extent) - axis_at - 1))

    factor_of = one(*pieces[0])
    for cut in pieces[1:]:
        factor_of = factor_of * one(*cut)
    return factor_of


def shared_out(stream_key, own, number, rows, count, top, limit, lean):
    order = jax.random.permutation(stream_key, count)
    crowded, common = portions_of(count, rows * top, limit, lean, True), portions_of(count, rows * top, limit, lean, False)
    places = jnp.arange(count)

    def named(tallies, turn):
        used = int((tallies > 0).sum())
        fixed = max(1, used // 4)
        passed = fixed + (places - fixed + turn * (used - fixed)) % max(1, count - fixed)
        return jnp.zeros((count,), jnp.int32).at[order[jnp.where(places < fixed, places, passed)]].set(jnp.asarray(tallies, jnp.int32))

    tallies = jnp.where(number % 4 == 0, named(crowded, number // 4), named(common, number - number // 4 - 1))
    mixed = jax.random.permutation(jax.random.fold_in(own, 3), count)
    giver, taker = mixed[0:count // 2 * 2:2], mixed[1:count // 2 * 2:2]
    room = jnp.minimum(tallies[giver] - 1, limit - tallies[taker]) // 2
    room = jnp.where((giver == order[0]) | (taker == order[0]) | (tallies[taker] == 0), 0, jnp.maximum(room, 0))
    passed = jax.random.randint(jax.random.fold_in(own, 4), (count // 2,), 0, 1 << 20) % (room + 1)
    tallies = tallies.at[giver].add(-passed).at[taker].add(passed)
    members = jnp.searchsorted(jnp.cumsum(tallies), jnp.arange(rows * top), side="right").astype(jnp.int32)
    listing = members.reshape(top, rows).T
    listing = listing[jax.random.permutation(jax.random.fold_in(own, 1), rows)]
    turn = jax.random.randint(jax.random.fold_in(own, 2), (rows, 1), 0, top)
    return jnp.take_along_axis(listing, (jnp.arange(top)[None, :] + turn) % top, axis=1)


def portions_of(count, total, limit, slope, full):
    portions = [(1 << 20) // math.isqrt(grade ** slope) + 1 for grade in range(1, count + 1)]
    largest = limit if full else min(limit, max(-(-total // count), total * portions[0] // sum(portions)))
    least = 1 if total - largest >= count - 1 else 0
    holding, rest = [largest] + [least] * (count - 1), total - largest - least * (count - 1)
    while rest > 0:
        candidates = [i for i in range(1, count) if holding[i] < largest] or [i for i in range(1, count) if holding[i] < limit]
        pool, left = sum([portions[i] for i in candidates]), rest
        for i in candidates:
            more = min(limit - holding[i], max(1, left * portions[i] // pool), rest)
            holding[i] = holding[i] + more
            rest = rest - more
    return np.array(holding)


def noise(own_key, shape, deviation, limit, pieces=(), held_as=jnp.bfloat16):
    array = deviation * jax.random.normal(own_key, shape, jnp.float32)
    if pieces:
        array = array * levels(own_key, shape, pieces, -0.22, 0.18)
    return jnp.clip(array, -limit, limit).astype(held_as)


def setup_inputs(seed: int = 0) -> dict:
    streams_of = jax.random.split(jax.random.key(seed), 12)
    resid = noise(streams_of[0], (TOKENS, D), 1.0, 6.0, ((0, 64),))
    pool_in = noise(streams_of[1], (TOKENS, POOLW), 1.0, 6.0, ((0, 64), (1, 4)))
    pool_mix = noise(streams_of[2], (GROUPS, PCH, PCH), PCH ** -0.5, 0.375, ((0, 4),))
    pool_gain = jnp.clip(1.0 + 0.18 * jax.random.normal(streams_of[3], (POOLW,), jnp.float32), 0.1, 1.9)
    out_proj = noise(streams_of[4], (POOLW, D), POOLW ** -0.5, 0.1875, ((0, 4),))
    norm_gain = jnp.clip(1.0 + 0.18 * jax.random.normal(streams_of[5], (D,), jnp.float32), 0.1, 1.9)
    w_gate = noise(streams_of[6], (EXPERTS, D, FF), D ** -0.5, 0.09375, ((0, 64), (2, 4)))
    w_up = noise(streams_of[7], (EXPERTS, D, FF), D ** -0.5, 0.09375, ((0, 64), (2, 4)))
    w_down = noise(streams_of[8], (EXPERTS, FF, D), FF ** -0.5, 0.1875, ((0, 64), (1, 4)))
    routes_keys = jax.random.split(jax.random.fold_in(streams_of[9], 1), TOKENS // TOK_SUB)
    routes_turns = jax.random.permutation(jax.random.fold_in(streams_of[9], 3), TOKENS // TOK_SUB)
    routes = jax.vmap(lambda own, number: shared_out(jax.random.fold_in(streams_of[9], 2), own, number, TOK_SUB, EXPERTS, TOP, CAP, 2))(routes_keys, routes_turns).reshape((TOKENS, TOP))
    route_weight = jnp.clip(jnp.exp(math.log(2.5) - 2.3025851 * jax.random.uniform(streams_of[10], (TOKENS, TOP), jnp.float32) ** levels(streams_of[10], (TOKENS, TOP), ((0, 64),), -0.2, 0.2)), 0.25, 2.5)
    return {"resid": resid, "pool_in": pool_in, "pool_mix": pool_mix, "pool_gain": pool_gain, "out_proj": out_proj, "norm_gain": norm_gain, "w_gate": w_gate, "w_up": w_up, "w_down": w_down, "routes": routes, "route_weight": route_weight}


EPS = 1e-06

def rounded(value):
    return lax.optimization_barrier(value.astype(jnp.bfloat16)).astype(jnp.float32)

def window_diff(block, width):
    row_count = block.shape[0]
    data = block.astype(jnp.float32)
    padded = jnp.concatenate([jnp.zeros((width - 1, data.shape[1]), jnp.float32), data], axis=0)
    total = jnp.zeros_like(data)
    for offset in range(width):
        total = total + padded[width - 1 - offset:width - 1 - offset + row_count]
    counted = jnp.minimum(jnp.arange(1, row_count + 1, dtype=jnp.float32), float(width))
    return (total / counted[:, None] - data).astype(jnp.bfloat16)

def reference(resid, pool_in, pool_mix, pool_gain, out_proj, norm_gain, w_gate, w_up, w_down, routes, route_weight):
    proj = jnp.zeros((TOKENS, D), jnp.float32)
    for group in range(GROUPS):
        lower = group * PCH
        diff = window_diff(pool_in[:, lower:lower + PCH], 2 ** (group + 1))
        pooled = (jnp.dot(diff, pool_mix[group], preferred_element_type=jnp.float32) * pool_gain[lower:lower + PCH]).astype(jnp.bfloat16)
        proj = proj + rounded(jnp.dot(pooled, out_proj[lower:lower + PCH], preferred_element_type=jnp.float32))
    proj = rounded(proj)
    mixed = resid.astype(jnp.float32) + proj
    scale = lax.rsqrt(lax.optimization_barrier(jnp.mean(mixed * mixed, axis=1, keepdims=True)) + EPS)
    normed = (mixed * scale * norm_gain).astype(jnp.bfloat16)
    normed_ext = jnp.concatenate([normed, jnp.zeros((1, D), jnp.bfloat16)], axis=0)
    flat_expert = routes.reshape(-1)
    flat_weight = route_weight.reshape(-1)
    flat_token = (jnp.arange(TOKENS * TOP, dtype=jnp.int32) // TOP).astype(jnp.int32)
    most = TOKENS // TOK_SUB * CAP

    def one_expert(total, expert):
        match = flat_expert == expert
        position = jnp.cumsum(match.astype(jnp.int32)) - 1
        slot = jnp.where(match, position, most).astype(jnp.int32)
        owner = jnp.full((most + 1,), TOKENS, jnp.int32).at[slot].set(flat_token)[:most]
        weight = jnp.zeros((most + 1,), jnp.float32).at[slot].set(flat_weight)[:most]
        inputs = normed_ext[owner]
        gate = jnp.dot(inputs, w_gate[expert], preferred_element_type=jnp.float32)
        upper = jnp.dot(inputs, w_up[expert], preferred_element_type=jnp.float32)
        hidden = (jax.nn.silu(gate) * upper).astype(jnp.bfloat16)
        down = w_down[expert]
        result = jnp.zeros((most, D), jnp.float32)
        for block in range(N_TP):
            lower = block * FF_PART
            result = result + rounded(jnp.dot(hidden[:, lower:lower + FF_PART], down[lower:lower + FF_PART], preferred_element_type=jnp.float32))
        total = total.at[owner].add(result * weight[:, None])
        return (total, None)
    moe, unused = lax.scan(one_expert, jnp.zeros((TOKENS + 1, D), jnp.float32), jnp.arange(EXPERTS, dtype=jnp.int32))
    return (mixed + moe[:TOKENS]).astype(jnp.bfloat16)
```

```python
import jax
import jax.numpy as jnp
from jax import lax
from jax.sharding import PartitionSpec as P

GROUPS = 4
HALVES = 2
CAP = 4
BLOCK = 64
EPS = 1e-06


def turned(x, axis, by):
    count = lax.axis_size(axis)
    return lax.ppermute(x, axis, [(i, (i + by) % count) for i in range(count)])


def piece(x, index, size, dim):
    return lax.dynamic_slice_in_dim(x, index * size, size, dim)


def rounded(value):
    return lax.optimization_barrier(value.astype(jnp.bfloat16)).astype(jnp.float32)


def group_diff(pool_in):
    row_count = pool_in.shape[0]
    reach = 2**GROUPS
    count = lax.axis_size("sp")
    before = lax.ppermute(
        pool_in[row_count - reach :], "sp", [(i, i + 1) for i in range(count - 1)]
    )
    data = pool_in.astype(jnp.float32)
    total = jnp.concatenate([before.astype(jnp.float32), data], axis=0)
    group = lax.axis_index("tp")
    chosen = jnp.zeros_like(data)
    for step in range(GROUPS):
        by = 2**step
        total = total[by:] + total[:-by]
        start = total.shape[0] - row_count
        chosen = jnp.where(group == step, total[start:], chosen)
    width = jnp.left_shift(jnp.int32(2), group)
    place = lax.axis_index("sp") * row_count + jnp.arange(row_count, dtype=jnp.int32) + 1
    counted = jnp.minimum(place, width).astype(jnp.float32)
    return (chosen / counted[:, None] - data).astype(jnp.bfloat16)


def slot_targets(routes, experts):
    row_count, choose = routes.shape
    blocks = row_count // BLOCK
    flat = routes.reshape(blocks, BLOCK * choose)
    order = jnp.arange(BLOCK * choose, dtype=jnp.int32)
    same = (flat[:, :, None] == flat[:, None, :]) & (order[None, None, :] < order[None, :, None])
    position = jnp.sum(same.astype(jnp.int32), axis=2)
    per_half = blocks // HALVES
    block_ids = (jnp.arange(blocks, dtype=jnp.int32) % per_half)[:, None]
    return (flat * (per_half * CAP) + block_ids * CAP + position).reshape(row_count, choose)


def three_parts(value):
    high = lax.reduce_precision(value, 8, 7)
    rest = value - high
    middle = lax.reduce_precision(rest, 8, 7)
    return [p.astype(jnp.bfloat16) for p in (high, middle, rest - middle)]


def dot(a, b):
    return jnp.dot(a, b, preferred_element_type=jnp.float32)


def on_device(
    resid,
    pool_in,
    pool_mix,
    pool_gain,
    out_proj,
    norm_gain,
    w_gate,
    w_up,
    w_down,
    routes,
    route_weight,
):
    token_count, width = resid.shape
    choose = routes.shape[1]
    experts = lax.axis_size("sp")
    slices = lax.axis_size("tp")
    part_width = width // slices
    me = lax.axis_index("tp")
    others = (1, slices - 1, 2)
    peers = [(me + by) % slices for by in (0, *others)]

    diff = group_diff(pool_in)
    pooled = (dot(diff, pool_mix[0]) * pool_gain).astype(jnp.bfloat16)
    parts = [
        lax.optimization_barrier(dot(pooled, piece(out_proj, p, part_width, 1)).astype(jnp.bfloat16))
        for p in peers
    ]
    arrived = [parts[0]] + [turned(x, "tp", by) for x, by in zip(parts[1:], others)]
    proj = rounded(sum(x.astype(jnp.float32) for x in arrived))
    mixed = piece(resid, me, part_width, 1).astype(jnp.float32) + proj
    squares = jnp.sum(mixed * mixed, axis=1)
    squares = squares + sum(turned(squares, "tp", by) for by in others)
    scale = lax.rsqrt(squares / width + EPS)
    normed = (mixed * scale[:, None] * piece(norm_gain, me, part_width, 0)).astype(jnp.bfloat16)

    w_down, normed = lax.optimization_barrier((w_down[0], normed))
    downs = [piece(w_down, me, part_width, 1)] + [
        turned(piece(w_down, p, part_width, 1), "tp", by) for p, by in zip(peers[1:], others)
    ]

    targets = slot_targets(routes, experts)
    half = token_count // HALVES
    slots = experts * (half // BLOCK) * CAP
    slot_ids = jnp.arange(slots, dtype=jnp.int32)
    sources = [me, (me - 1) % slices, (me + 1) % slices, (me + 2) % slices]
    gates = [piece(w_gate[0], p, part_width, 0) for p in sources]
    ups = [piece(w_up[0], p, part_width, 0) for p in sources]

    moes = []
    for h in range(HALVES):
        wanted = targets[h * half : (h + 1) * half]
        weights = route_weight[h * half : (h + 1) * half]
        chosen = sum(
            (slot_ids[:, None] == wanted[None, :, k]).astype(jnp.bfloat16) for k in range(choose)
        )
        outgoing = dot(chosen, normed[h * half : (h + 1) * half]).astype(jnp.bfloat16)
        rows = lax.all_to_all(
            outgoing.reshape(experts, -1, part_width), "sp", 0, 0, tiled=True
        ).reshape(slots, part_width)
        before = turned(rows, "tp", 1)
        after = turned(rows, "tp", -1)
        far_low = turned(before[: slots // 2], "tp", 1)
        far_high = turned(after[slots // 2 :], "tp", -1)
        far = jnp.concatenate([far_low, far_high], axis=0)
        blocks = (rows, before, after, far)
        gate = sum(dot(x, w) for x, w in zip(blocks, gates))
        upper = sum(dot(x, w) for x, w in zip(blocks, ups))
        hidden = (jax.nn.silu(gate) * upper).astype(jnp.bfloat16)
        hiddens = [hidden] + [turned(hidden, "tp", by) for by in others]
        spread = sum(dot(x, w) for x, w in zip(hiddens, downs)).astype(jnp.bfloat16)
        returned = lax.all_to_all(
            spread.reshape(experts, -1, part_width), "sp", 0, 0, tiled=True
        ).reshape(slots, part_width)
        moe = 0.0
        places = [wanted[:, k, None] == slot_ids[None, :] for k in range(choose)]
        combine = sum(jnp.where(p, weights[:, k, None], 0.0) for k, p in enumerate(places))
        for share in three_parts(combine):
            moe = moe + dot(share, returned)
        moes.append(moe)
    result = (mixed + jnp.concatenate(moes, axis=0)).astype(jnp.bfloat16)
    final = lax.all_to_all(result.reshape(slices, -1, part_width), "tp", 0, 0, tiled=True)
    return jnp.moveaxis(final, 0, 1).reshape(-1, width)


def solution(mesh):
    in_specs = (
        P("sp", None),
        P("sp", "tp"),
        P("tp", None, None),
        P("tp"),
        P("tp", None),
        P(),
        P("sp", None, "tp"),
        P("sp", None, "tp"),
        P("sp", "tp", None),
        P("sp", None),
        P("sp", None),
    )
    out_specs = P(("sp", "tp"), None)
    return jax.shard_map(
        on_device, mesh=mesh, in_specs=in_specs, out_specs=out_specs, check_vma=False
    )
```

```python
import jax
import jax.numpy as jnp
from jax import lax
from jax.experimental import pallas as pl
from jax.experimental.pallas import tpu as pltpu
from jax.sharding import PartitionSpec as P


GROUPS = 4
HALVES = 2
CAP = 4
BLOCK = 64
EPS = 1e-06


def turned(x, by):
    count = lax.axis_size("tp")
    return lax.ppermute(x, "tp", [(i, (i + by) % count) for i in range(count)])


def piece(x, index, size, dim):
    return lax.dynamic_slice_in_dim(x, index * size, size, dim)


def rounded(value):
    return lax.optimization_barrier(value.astype(jnp.bfloat16)).astype(jnp.float32)


def pool_kernel(place, before, pool_in, mix, gain, proj, *outs_and_pooled):
    outs, pooled = outs_and_pooled[:-1], outs_and_pooled[-1]
    step = pl.program_id(0)
    group, first = place[0], place[1]
    row_count = pool_in.shape[0]

    @pl.when(step == 0)
    def _():
        data = pool_in[...].astype(jnp.float32)
        total = jnp.concatenate([before[...].astype(jnp.float32), data], axis=0)
        chosen = jnp.zeros_like(data)
        for at in range(GROUPS):
            by = 2**at
            total = total + jnp.concatenate([total[-by:], total[:-by]], axis=0)
            chosen = jnp.where(group == at, total[-row_count:], chosen)
        width = jnp.left_shift(jnp.int32(2), group)
        place_of = first + lax.broadcasted_iota(jnp.int32, data.shape, 0) + 1
        counted = jnp.minimum(place_of, width).astype(jnp.float32)
        diff = (chosen / counted - data).astype(jnp.bfloat16)
        pooled[...] = (dot(diff, mix[0]) * gain[...]).astype(jnp.bfloat16)

    part = dot(pooled[...], proj[...]).astype(jnp.bfloat16)
    for at, out in enumerate(outs):

        @pl.when(step == at)
        def _(out=out):
            out[...] = part


def pool_parts(pool_in, pool_mix, pool_gain, out_proj, order):
    row_count, channels = pool_in.shape
    reach = 2**GROUPS
    count = lax.axis_size("sp")
    before = lax.ppermute(
        pool_in[row_count - reach :], "sp", [(i, i + 1) for i in range(count - 1)]
    )
    slices = len(order)
    part_width = out_proj.shape[1] // slices
    place = jnp.stack([lax.axis_index("tp"), lax.axis_index("sp") * row_count, *order]).astype(
        jnp.int32
    )
    whole = lambda *shape: pl.BlockSpec(shape, lambda i, place: (0,) * len(shape))
    return pl.pallas_call(
        pool_kernel,
        grid_spec=pltpu.PrefetchScalarGridSpec(
            num_scalar_prefetch=1,
            grid=(slices,),
            in_specs=[
                whole(reach, channels),
                whole(row_count, channels),
                whole(1, channels, channels),
                whole(1, channels),
                pl.BlockSpec((channels, part_width), lambda i, place: (0, place[2 + i])),
            ],
            out_specs=[whole(row_count, part_width)] * slices,
            scratch_shapes=[pltpu.VMEM((row_count, channels), jnp.bfloat16)],
        ),
        out_shape=[jax.ShapeDtypeStruct((row_count, part_width), jnp.bfloat16)] * slices,
        cost_estimate=pl.CostEstimate(
            flops=2 * row_count * channels * (channels + slices * part_width),
            bytes_accessed=8 * channels * slices * part_width,
            transcendentals=0,
        ),
        name="pool",
    )(place, before, pool_in, pool_mix, pool_gain[None], out_proj)


def slot_targets(routes):
    row_count, choose = routes.shape
    blocks = row_count // BLOCK
    flat = routes.reshape(blocks, BLOCK * choose)
    order = jnp.arange(BLOCK * choose, dtype=jnp.int32)
    same = (flat[:, :, None] == flat[:, None, :]) & (order[None, None, :] < order[None, :, None])
    position = jnp.sum(same.astype(jnp.int32), axis=2)
    per_half = blocks // HALVES
    block_ids = (jnp.arange(blocks, dtype=jnp.int32) % per_half)[:, None]
    return (flat * (per_half * CAP) + block_ids * CAP + position).reshape(row_count, choose)


def three_parts(value):
    high = lax.reduce_precision(value, 8, 7)
    rest = value - high
    middle = lax.reduce_precision(rest, 8, 7)
    return [p.astype(jnp.bfloat16) for p in (high, middle, rest - middle)]


def dot(a, b):
    return jnp.dot(a, b, preferred_element_type=jnp.float32)


def spread_out(x):
    return lax.all_to_all(x, "sp", 0, 0, tiled=True)


def handed(result, by, first, blocks, sub):
    count = lax.axis_size("tp")
    target = (lax.axis_index("tp") + by) % count
    block = piece(result, jnp.clip(target - first, 0, blocks - 1), sub, 0)
    targets = range(first, first + blocks)
    return lax.ppermute(block, "tp", [((t - by) % count, t) for t in targets])


def partials_kernel(rows, own_w, before_w, after_w, far_w, forward, backward, on, back, own):
    mid = rows.shape[0] // 2
    x = rows[...]
    far = dot(x, far_w[...]).astype(jnp.bfloat16)
    forward[:mid] = far[:mid]
    backward[:mid] = far[mid:]
    after = dot(x, after_w[...])
    forward[mid:] = after[mid:].astype(jnp.bfloat16)
    on[...] = after[:mid]
    before = dot(x, before_w[...])
    backward[mid:] = before[:mid].astype(jnp.bfloat16)
    back[...] = before[mid:]
    own[...] = dot(x, own_w[...])


def partials(rows, own_w, before_w, after_w, far_w):
    count, depth = rows.shape
    units = own_w.shape[1]
    block = units // 2
    mid = count // 2
    weight = pl.BlockSpec((depth, block), lambda i: (0, i))
    return pl.pallas_call(
        partials_kernel,
        grid=(units // block,),
        in_specs=[pl.BlockSpec((count, depth), lambda i: (0, 0))] + [weight] * 4,
        out_specs=[
            pl.BlockSpec((count, block), lambda i: (0, i)),
            pl.BlockSpec((count, block), lambda i: (0, i)),
            pl.BlockSpec((mid, block), lambda i: (0, i)),
            pl.BlockSpec((mid, block), lambda i: (0, i)),
            pl.BlockSpec((count, block), lambda i: (0, i)),
        ],
        out_shape=[
            jax.ShapeDtypeStruct((count, units), jnp.bfloat16),
            jax.ShapeDtypeStruct((count, units), jnp.bfloat16),
            jax.ShapeDtypeStruct((mid, units), jnp.float32),
            jax.ShapeDtypeStruct((mid, units), jnp.float32),
            jax.ShapeDtypeStruct((count, units), jnp.float32),
        ],
        cost_estimate=pl.CostEstimate(
            flops=8 * count * depth * units, bytes_accessed=10 * depth * units, transcendentals=0
        ),
        name="partials",
    )(rows, own_w, before_w, after_w, far_w)


def on_device(
    resid,
    pool_in,
    pool_mix,
    pool_gain,
    out_proj,
    norm_gain,
    w_gate,
    w_up,
    w_down,
    routes,
    route_weight,
):
    token_count, width = resid.shape
    choose = routes.shape[1]
    experts = lax.axis_size("sp")
    slices = lax.axis_size("tp")
    part_width = width // slices
    me = lax.axis_index("tp")
    others = (1, slices - 1, 2)
    peers = [(me + by) % slices for by in (0, *others)]

    parts = pool_parts(pool_in, pool_mix, pool_gain, out_proj, peers)
    arrived = [parts[0]] + [turned(x, by) for x, by in zip(parts[1:], others)]
    proj = rounded(sum(x.astype(jnp.float32) for x in arrived))
    mixed = piece(resid, me, part_width, 1).astype(jnp.float32) + proj
    squares = jnp.sum(mixed * mixed, axis=1)

    def resplit(cut):
        return [cut(me)] + [turned(cut(p), by) for p, by in zip(peers[1:], others)]

    downs = resplit(lambda p: piece(w_down[0], p, part_width, 1))
    gate_ups = resplit(
        lambda p: jnp.concatenate(
            [piece(w_gate[0], p, part_width, 0), piece(w_up[0], p, part_width, 0)], axis=1
        ),
    )
    squares = squares + sum(turned(squares, by) for by in others)
    scale = lax.rsqrt(squares / width + EPS)
    normed = (mixed * scale[:, None] * piece(norm_gain, me, part_width, 0)).astype(jnp.bfloat16)

    targets = slot_targets(routes)
    half = token_count // HALVES
    slots = experts * (half // BLOCK) * CAP
    slot_ids = jnp.arange(slots, dtype=jnp.int32)
    sub = token_count // slices
    finals = []
    for h in range(HALVES):
        wanted = targets[h * half : (h + 1) * half]
        weights = route_weight[h * half : (h + 1) * half]
        chosen = sum(
            (slot_ids[:, None] == wanted[None, :, k]).astype(jnp.bfloat16) for k in range(choose)
        )
        outgoing = dot(chosen, normed[h * half : (h + 1) * half]).astype(jnp.bfloat16)
        rows = spread_out(outgoing.reshape(experts, -1, part_width))
        rows = rows.reshape(slots, part_width)
        low, high = slice(0, slots // 2), slice(slots // 2, slots)
        forward, backward, on, back, own = partials(rows, *gate_ups)
        from_before = turned(forward, 1).astype(jnp.float32)
        from_after = turned(backward, -1).astype(jnp.float32)
        relay_on = (on + from_before[low]).astype(jnp.bfloat16)
        relay_back = (back + from_after[low]).astype(jnp.bfloat16)
        last_low = turned(relay_on, 1).astype(jnp.float32)
        last_high = turned(relay_back, -1).astype(jnp.float32)
        gate_up = jnp.concatenate(
            [
                own[low] + from_after[high] + last_low,
                own[high] + from_before[high] + last_high,
            ],
            axis=0,
        )
        gate, upper = jnp.split(gate_up, 2, axis=1)
        hidden = (jax.nn.silu(gate) * upper).astype(jnp.bfloat16)
        hiddens = [hidden] + [turned(hidden, by) for by in others]
        spread = dot(jnp.concatenate(hiddens, axis=1), jnp.concatenate(downs, axis=0))
        spread = spread.astype(jnp.bfloat16)
        returned = spread_out(spread.reshape(experts, -1, part_width))
        if finals:
            *finals[0], returned = lax.optimization_barrier((*finals[0], returned))
        returned = returned.reshape(slots, part_width)
        places = [wanted[:, k, None] == slot_ids[None, :] for k in range(choose)]
        combine = sum(jnp.where(p, weights[:, k, None], 0.0) for k, p in enumerate(places))
        shares = dot(jnp.concatenate(three_parts(combine), axis=0), returned)
        moe = jnp.sum(shares.reshape(3, half, part_width), axis=0)
        result = (mixed[h * half : (h + 1) * half] + moe).astype(jnp.bfloat16)
        blocks = half // sub
        finals.append(
            [piece(result, jnp.clip(me - h * blocks, 0, blocks - 1), sub, 0)]
            + [handed(result, by, h * blocks, blocks, sub) for by in others]
        )
    mine = [jnp.where(me * sub < half, a, b) for a, b in zip(*finals)]
    sources = [(me - by) % slices for by in (0, *others)]
    columns = [
        sum(jnp.where(o == source, x, jnp.zeros_like(x)) for o, x in zip(sources, mine))
        for source in range(slices)
    ]
    return jnp.concatenate(columns, axis=1)


def solution(mesh):
    in_specs = (
        P("sp", None),
        P("sp", "tp"),
        P("tp", None, None),
        P("tp"),
        P("tp", None),
        P(),
        P("sp", None, "tp"),
        P("sp", None, "tp"),
        P("sp", "tp", None),
        P("sp", None),
        P("sp", None),
    )
    out_specs = P(("sp", "tp"), None)
    return jax.shard_map(
        on_device, mesh=mesh, in_specs=in_specs, out_specs=out_specs, check_vma=False
    )
```

```python
import jax
import jax.numpy as jnp
from jax import lax
from jax.experimental import pallas as pl
from jax.experimental.pallas import tpu as pltpu
from jax.sharding import PartitionSpec as P


GROUPS = 4
HALVES = 2
CAP = 4
BLOCK = 64
EPS = 1e-06


def turned(x, by):
    count = lax.axis_size("tp")
    return lax.ppermute(x, "tp", [(i, (i + by) % count) for i in range(count)])


def piece(x, index, size, dim):
    return lax.dynamic_slice_in_dim(x, index * size, size, dim)


def rounded(value):
    return lax.optimization_barrier(value.astype(jnp.bfloat16)).astype(jnp.float32)


def pool_kernel(place, before, pool_in, mix, gain, pooled):
    group, first, core = place[0], place[1], place[2]
    row_count, channels = pool_in.shape
    data = pool_in[...].astype(jnp.float32)
    total = jnp.concatenate([before[...].astype(jnp.float32), data], axis=0)
    chosen = jnp.zeros_like(data)
    for at in range(GROUPS):
        by = 2**at
        total = total + jnp.concatenate([total[-by:], total[:-by]], axis=0)
        chosen = jnp.where(group == at, total[-row_count:], chosen)
    width = jnp.left_shift(jnp.int32(2), group)
    place_of = first + lax.broadcasted_iota(jnp.int32, data.shape, 0) + 1
    counted = jnp.minimum(place_of, width).astype(jnp.float32)
    diff = (chosen / counted - data).astype(jnp.bfloat16)
    result = (dot(diff, mix[0]) * gain[...]).astype(jnp.bfloat16)
    half = channels // 2
    low, high = result[:, :half], result[:, half:]
    pooled[:, :half] = jnp.where(core == 0, low, high)
    pooled[:, half:] = jnp.where(core == 0, high, low)


def pooled_channels(pool_in, pool_mix, pool_gain, core):
    row_count, channels = pool_in.shape
    reach = 2**GROUPS
    count = lax.axis_size("sp")
    before = lax.ppermute(
        pool_in[row_count - reach :], "sp", [(i, i + 1) for i in range(count - 1)]
    )
    place = jnp.stack([lax.axis_index("tp"), lax.axis_index("sp") * row_count, core])
    vmem = pl.BlockSpec(memory_space=pltpu.VMEM)
    return pl.pallas_call(
        pool_kernel,
        in_specs=[pl.BlockSpec(memory_space=pltpu.SMEM)] + [vmem] * 4,
        out_specs=vmem,
        out_shape=jax.ShapeDtypeStruct((row_count, channels), jnp.bfloat16),
        cost_estimate=pl.CostEstimate(
            flops=2 * row_count * channels * channels,
            bytes_accessed=6 * row_count * channels,
            transcendentals=0,
        ),
        name="pool",
    )(place.astype(jnp.int32), before, pool_in, pool_mix, pool_gain[None])


def slot_targets(routes):
    row_count, choose = routes.shape
    blocks = row_count // BLOCK
    flat = routes.reshape(blocks, BLOCK * choose)
    order = jnp.arange(BLOCK * choose, dtype=jnp.int32)
    same = (flat[:, :, None] == flat[:, None, :]) & (order[None, None, :] < order[None, :, None])
    position = jnp.sum(same.astype(jnp.int32), axis=2)
    per_half = blocks // HALVES
    block_ids = (jnp.arange(blocks, dtype=jnp.int32) % per_half)[:, None]
    return (flat * (per_half * CAP) + block_ids * CAP + position).reshape(row_count, choose)


def three_parts(value):
    high = lax.reduce_precision(value, 8, 7)
    rest = value - high
    middle = lax.reduce_precision(rest, 8, 7)
    return [p.astype(jnp.bfloat16) for p in (high, middle, rest - middle)]


def dot(a, b):
    return jnp.dot(a, b, preferred_element_type=jnp.float32)


def spread_out(x):
    return lax.all_to_all(x, "sp", 0, 0, tiled=True)


def handed(result, by, first, blocks, sub):
    count = lax.axis_size("tp")
    target = (lax.axis_index("tp") + by) % count
    block = piece(result, jnp.clip(target - first, 0, blocks - 1), sub, 0)
    targets = range(first, first + blocks)
    return lax.ppermute(block, "tp", [((t - by) % count, t) for t in targets])


def partials_kernel(rows, own_w, before_w, after_w, far_w, forward, backward, on, back, own):
    mid = rows.shape[0] // 2
    x = rows[...]
    far = dot(x, far_w[...]).astype(jnp.bfloat16)
    forward[:mid] = far[:mid]
    backward[:mid] = far[mid:]
    after = dot(x, after_w[...])
    forward[mid:] = after[mid:].astype(jnp.bfloat16)
    on[...] = after[:mid]
    before = dot(x, before_w[...])
    backward[mid:] = before[:mid].astype(jnp.bfloat16)
    back[...] = before[mid:]
    own[...] = dot(x, own_w[...])


def partials(rows, own_w, before_w, after_w, far_w):
    count, depth = rows.shape
    units = own_w.shape[1]
    block = units // 2
    mid = count // 2
    weight = pl.BlockSpec((depth, block), lambda i: (0, i))
    return pl.pallas_call(
        partials_kernel,
        grid=(units // block,),
        in_specs=[pl.BlockSpec((count, depth), lambda i: (0, 0))] + [weight] * 4,
        out_specs=[
            pl.BlockSpec((count, block), lambda i: (0, i)),
            pl.BlockSpec((count, block), lambda i: (0, i)),
            pl.BlockSpec((mid, block), lambda i: (0, i)),
            pl.BlockSpec((mid, block), lambda i: (0, i)),
            pl.BlockSpec((count, block), lambda i: (0, i)),
        ],
        out_shape=[
            jax.ShapeDtypeStruct((count, units), jnp.bfloat16),
            jax.ShapeDtypeStruct((count, units), jnp.bfloat16),
            jax.ShapeDtypeStruct((mid, units), jnp.float32),
            jax.ShapeDtypeStruct((mid, units), jnp.float32),
            jax.ShapeDtypeStruct((count, units), jnp.float32),
        ],
        cost_estimate=pl.CostEstimate(
            flops=8 * count * depth * units, bytes_accessed=10 * depth * units, transcendentals=0
        ),
        name="partials",
    )(rows, own_w, before_w, after_w, far_w)


def on_device(
    resid,
    pool_in,
    pool_mix,
    pool_gain,
    out_proj,
    norm_gain,
    w_gate,
    w_up,
    w_down,
    routes,
    route_weight,
):
    token_count, width = resid.shape
    choose = routes.shape[1]
    experts = lax.axis_size("sp")
    slices = lax.axis_size("tp")
    part_width = width // slices
    me = lax.axis_index("tp")
    others = (1, slices - 1, 2)
    peers = [(me + by) % slices for by in (0, *others)]

    core = lax.axis_index("sp") % 2
    group_rows = out_proj.shape[0] // 2

    def columns(rows, peer):
        return piece(piece(out_proj, rows, group_rows, 0), peer, part_width, 1)

    fetched = [turned(columns(core, p), by) for p, by in zip(peers[1:], others)]
    pooled = pooled_channels(pool_in, pool_mix, pool_gain, core)
    w_down, w_gate, w_up, pooled = lax.optimization_barrier((w_down, w_gate, w_up, pooled))
    pooleds = [pooled] + [turned(pooled, by) for by in others]
    fetched = jnp.concatenate(fetched, axis=0)
    swapped = lax.ppermute(fetched, "sp", [(i, i ^ 1) for i in range(experts)])
    proj = dot(
        jnp.concatenate([x[:, :group_rows] for x in pooleds], axis=1),
        jnp.concatenate([columns(core, me), fetched], axis=0),
    ) + dot(
        jnp.concatenate([x[:, group_rows:] for x in pooleds], axis=1),
        jnp.concatenate([columns(1 - core, me), swapped], axis=0),
    )
    proj = rounded(proj)
    mixed = piece(resid, me, part_width, 1).astype(jnp.float32) + proj
    squares = jnp.sum(mixed * mixed, axis=1)

    def resplit(cut):
        own = cut(me)
        return [own] + [turned(cut(p), by) for p, by in zip(peers[1:], others)]

    downs = resplit(lambda p: piece(w_down[0], p, part_width, 1))
    gate_ups = resplit(
        lambda p: jnp.concatenate(
            [piece(w_gate[0], p, part_width, 0), piece(w_up[0], p, part_width, 0)], axis=1
        ),
    )
    squares = squares + sum(turned(squares, by) for by in others)
    scale = lax.rsqrt(squares / width + EPS)
    normed = (mixed * scale[:, None] * piece(norm_gain, me, part_width, 0)).astype(jnp.bfloat16)

    targets = slot_targets(routes)
    half = token_count // HALVES
    slots = experts * (half // BLOCK) * CAP
    slot_ids = jnp.arange(slots, dtype=jnp.int32)
    sub = token_count // slices
    finals = []
    for h in range(HALVES):
        wanted = targets[h * half : (h + 1) * half]
        weights = route_weight[h * half : (h + 1) * half]
        chosen = sum(
            (slot_ids[:, None] == wanted[None, :, k]).astype(jnp.bfloat16) for k in range(choose)
        )
        outgoing = dot(chosen, normed[h * half : (h + 1) * half]).astype(jnp.bfloat16)
        rows = spread_out(outgoing.reshape(experts, -1, part_width))
        rows = rows.reshape(slots, part_width)
        low, high = slice(0, slots // 2), slice(slots // 2, slots)
        forward, backward, on, back, own = partials(rows, *gate_ups)
        from_before = turned(forward, 1)
        from_after = turned(backward, -1)
        relay_on = (on + from_before[low].astype(jnp.float32)).astype(jnp.bfloat16)
        relay_back = (back + from_after[low].astype(jnp.float32)).astype(jnp.bfloat16)
        last_low = turned(relay_on, 1)
        last_high = turned(relay_back, -1)
        gate_up = jnp.concatenate(
            [
                own[low] + from_after[high].astype(jnp.float32) + last_low.astype(jnp.float32),
                own[high] + from_before[high].astype(jnp.float32) + last_high.astype(jnp.float32),
            ],
            axis=0,
        )
        gate, upper = jnp.split(gate_up, 2, axis=1)
        hidden = (jax.nn.silu(gate) * upper).astype(jnp.bfloat16)
        hiddens = [hidden] + [turned(hidden, by) for by in others]
        spread = dot(jnp.concatenate(hiddens, axis=1), jnp.concatenate(downs, axis=0))
        spread = spread.astype(jnp.bfloat16)
        returned = spread_out(spread.reshape(experts, -1, part_width))
        if finals:
            *finals[0], returned = lax.optimization_barrier((*finals[0], returned))
        returned = returned.reshape(slots, part_width)
        places = [wanted[:, k, None] == slot_ids[None, :] for k in range(choose)]
        combine = sum(jnp.where(p, weights[:, k, None], 0.0) for k, p in enumerate(places))
        shares = dot(jnp.concatenate(three_parts(combine), axis=0), returned)
        moe = jnp.sum(shares.reshape(3, half, part_width), axis=0)
        result = (mixed[h * half : (h + 1) * half] + moe).astype(jnp.bfloat16)
        blocks = half // sub
        finals.append(
            [piece(result, jnp.clip(me - h * blocks, 0, blocks - 1), sub, 0)]
            + [handed(result, by, h * blocks, blocks, sub) for by in others]
        )
    mine = [jnp.where(me * sub < half, a, b) for a, b in zip(*finals)]
    sources = [(me - by) % slices for by in (0, *others)]
    columns = [
        sum(jnp.where(o == source, x, jnp.zeros_like(x)) for o, x in zip(sources, mine))
        for source in range(slices)
    ]
    return jnp.concatenate(columns, axis=1)


def solution(mesh):
    in_specs = (
        P("sp", None),
        P("sp", "tp"),
        P("tp", None, None),
        P("tp"),
        P("tp", None),
        P(),
        P("sp", None, "tp"),
        P("sp", None, "tp"),
        P("sp", "tp", None),
        P("sp", None),
        P("sp", None),
    )
    out_specs = P(("sp", "tp"), None)
    return jax.shard_map(
        on_device, mesh=mesh, in_specs=in_specs, out_specs=out_specs, check_vma=False
    )
```

```python
import jax
import jax.numpy as jnp
from jax import lax
from jax.experimental import pallas as pl
from jax.experimental.pallas import tpu as pltpu
from jax.sharding import PartitionSpec as P


GROUPS = 4
HALVES = 2
CAP = 4
BLOCK = 64
EPS = 1e-06


def turned(x, by):
    count = lax.axis_size("tp")
    return lax.ppermute(x, "tp", [(i, (i + by) % count) for i in range(count)])


def piece(x, index, size, dim):
    return lax.dynamic_slice_in_dim(x, index * size, size, dim)


def rounded(value):
    return lax.optimization_barrier(value.astype(jnp.bfloat16)).astype(jnp.float32)


def pool_kernel(place, before, pool_in, mix, gain, pooled):
    group, first, core = place[0], place[1], place[2]
    row_count, channels = pool_in.shape
    data = pool_in[...].astype(jnp.float32)
    total = jnp.concatenate([before[...].astype(jnp.float32), data], axis=0)
    chosen = jnp.zeros_like(data)
    for at in range(GROUPS):
        by = 2**at
        total = total + jnp.concatenate([total[-by:], total[:-by]], axis=0)
        chosen = jnp.where(group == at, total[-row_count:], chosen)
    width = jnp.left_shift(jnp.int32(2), group)
    place_of = first + lax.broadcasted_iota(jnp.int32, data.shape, 0) + 1
    counted = jnp.minimum(place_of, width).astype(jnp.float32)
    diff = (chosen / counted - data).astype(jnp.bfloat16)
    result = (dot(diff, mix[0]) * gain[...]).astype(jnp.bfloat16)
    half = channels // 2
    low, high = result[:, :half], result[:, half:]
    pooled[:, :half] = jnp.where(core == 0, low, high)
    pooled[:, half:] = jnp.where(core == 0, high, low)


def pooled_channels(pool_in, pool_mix, pool_gain, core):
    row_count, channels = pool_in.shape
    reach = 2**GROUPS
    count = lax.axis_size("sp")
    before = lax.ppermute(
        pool_in[row_count - reach :], "sp", [(i, i + 1) for i in range(count - 1)]
    )
    place = jnp.stack([lax.axis_index("tp"), lax.axis_index("sp") * row_count, core])
    vmem = pl.BlockSpec(memory_space=pltpu.VMEM)
    return pl.pallas_call(
        pool_kernel,
        in_specs=[pl.BlockSpec(memory_space=pltpu.SMEM)] + [vmem] * 4,
        out_specs=vmem,
        out_shape=jax.ShapeDtypeStruct((row_count, channels), jnp.bfloat16),
        cost_estimate=pl.CostEstimate(
            flops=2 * row_count * channels * channels,
            bytes_accessed=6 * row_count * channels,
            transcendentals=0,
        ),
        name="pool",
    )(place.astype(jnp.int32), before, pool_in, pool_mix, pool_gain[None])


def slot_targets(routes):
    row_count, choose = routes.shape
    blocks = row_count // BLOCK
    flat = routes.reshape(blocks, BLOCK * choose)
    order = jnp.arange(BLOCK * choose, dtype=jnp.int32)
    same = (flat[:, :, None] == flat[:, None, :]) & (order[None, None, :] < order[None, :, None])
    position = jnp.sum(same.astype(jnp.int32), axis=2)
    per_half = blocks // HALVES
    block_ids = (jnp.arange(blocks, dtype=jnp.int32) % per_half)[:, None]
    return (flat * (per_half * CAP) + block_ids * CAP + position).reshape(row_count, choose)


def three_parts(value):
    high = lax.reduce_precision(value, 8, 7)
    rest = value - high
    middle = lax.reduce_precision(rest, 8, 7)
    return [p.astype(jnp.bfloat16) for p in (high, middle, rest - middle)]


def dot(a, b):
    return jnp.dot(a, b, preferred_element_type=jnp.float32)


def spread_out(x):
    return lax.all_to_all(x, "sp", 0, 0, tiled=True)


def handed(result, by, first, blocks, sub):
    count = lax.axis_size("tp")
    target = (lax.axis_index("tp") + by) % count
    block = piece(result, jnp.clip(target - first, 0, blocks - 1), sub, 0)
    targets = range(first, first + blocks)
    return lax.ppermute(block, "tp", [((t - by) % count, t) for t in targets])


def partials_kernel(rows, own_w, before_w, after_w, far_w, forward, backward, on, back, own):
    mid = rows.shape[0] // 2
    x = rows[...]
    far = dot(x, far_w[...]).astype(jnp.bfloat16)
    forward[:mid] = far[:mid]
    backward[:mid] = far[mid:]
    after = dot(x, after_w[...])
    forward[mid:] = after[mid:].astype(jnp.bfloat16)
    on[...] = after[:mid]
    before = dot(x, before_w[...])
    backward[mid:] = before[:mid].astype(jnp.bfloat16)
    back[...] = before[mid:]
    own[...] = dot(x, own_w[...])


def partials(rows, own_w, before_w, after_w, far_w):
    count, depth = rows.shape
    units = own_w.shape[1]
    block = units // 2
    mid = count // 2
    weight = pl.BlockSpec((depth, block), lambda i: (0, i))
    return pl.pallas_call(
        partials_kernel,
        grid=(units // block,),
        in_specs=[pl.BlockSpec((count, depth), lambda i: (0, 0))] + [weight] * 4,
        out_specs=[
            pl.BlockSpec((count, block), lambda i: (0, i)),
            pl.BlockSpec((count, block), lambda i: (0, i)),
            pl.BlockSpec((mid, block), lambda i: (0, i)),
            pl.BlockSpec((mid, block), lambda i: (0, i)),
            pl.BlockSpec((count, block), lambda i: (0, i)),
        ],
        out_shape=[
            jax.ShapeDtypeStruct((count, units), jnp.bfloat16),
            jax.ShapeDtypeStruct((count, units), jnp.bfloat16),
            jax.ShapeDtypeStruct((mid, units), jnp.float32),
            jax.ShapeDtypeStruct((mid, units), jnp.float32),
            jax.ShapeDtypeStruct((count, units), jnp.float32),
        ],
        cost_estimate=pl.CostEstimate(
            flops=8 * count * depth * units, bytes_accessed=10 * depth * units, transcendentals=0
        ),
        name="partials",
    )(rows, own_w, before_w, after_w, far_w)


def in_order(values, sources):
    return [
        sum(jnp.where(source == at, x, jnp.zeros_like(x)) for source, x in zip(sources, values))
        for at in range(len(values))
    ]


def on_device(
    resid,
    pool_in,
    pool_mix,
    pool_gain,
    out_proj,
    norm_gain,
    w_gate,
    w_up,
    w_down,
    routes,
    route_weight,
):
    token_count, width = resid.shape
    choose = routes.shape[1]
    experts = lax.axis_size("sp")
    slices = lax.axis_size("tp")
    part_width = width // slices
    me = lax.axis_index("tp")
    others = (1, slices - 1, 2)
    peers = [(me + by) % slices for by in (0, *others)]

    core = lax.axis_index("sp") % 2
    group_rows = out_proj.shape[0] // 2

    def columns(rows):
        picked = piece(out_proj, rows, group_rows, 0)
        return jnp.moveaxis(picked.reshape(group_rows, slices, part_width), 1, 0)

    fetched = lax.all_to_all(columns(core), "tp", 0, 0, tiled=True)
    fetched = fetched.reshape(slices * group_rows, part_width)
    pooled = pooled_channels(pool_in, pool_mix, pool_gain, core)
    w_down, w_gate, w_up, pooled = lax.optimization_barrier((w_down, w_gate, w_up, pooled))
    rotated = [pooled] + [turned(pooled, by) for by in others]
    sources = [(me - by) % slices for by in (0, *others)]
    pooleds = in_order(rotated, sources)
    swapped = lax.ppermute(fetched, "sp", [(i, i ^ 1) for i in range(experts)])
    proj = dot(jnp.concatenate([x[:, :group_rows] for x in pooleds], axis=1), fetched) + dot(
        jnp.concatenate([x[:, group_rows:] for x in pooleds], axis=1), swapped
    )
    proj = rounded(proj)
    mixed = piece(resid, me, part_width, 1).astype(jnp.float32) + proj
    squares = jnp.sum(mixed * mixed, axis=1)

    def resplit(cut):
        own = cut(me)
        return [own] + [turned(cut(p), by) for p, by in zip(peers[1:], others)]

    downs = resplit(lambda p: piece(w_down[0], p, part_width, 1))
    gate_ups = resplit(
        lambda p: jnp.concatenate(
            [piece(w_gate[0], p, part_width, 0), piece(w_up[0], p, part_width, 0)], axis=1
        ),
    )
    squares = squares + sum(turned(squares, by) for by in others)
    scale = lax.rsqrt(squares / width + EPS)
    normed = (mixed * scale[:, None] * piece(norm_gain, me, part_width, 0)).astype(jnp.bfloat16)

    downs = lax.optimization_barrier(jnp.concatenate(downs, axis=0))
    targets = slot_targets(routes)
    half = token_count // HALVES
    slots = experts * (half // BLOCK) * CAP
    slot_ids = jnp.arange(slots, dtype=jnp.int32)
    sub = token_count // slices
    finals = []
    for h in range(HALVES):
        wanted = targets[h * half : (h + 1) * half]
        weights = route_weight[h * half : (h + 1) * half]
        chosen = sum(
            (slot_ids[:, None] == wanted[None, :, k]).astype(jnp.bfloat16) for k in range(choose)
        )
        outgoing = dot(chosen, normed[h * half : (h + 1) * half]).astype(jnp.bfloat16)
        rows = spread_out(outgoing.reshape(experts, -1, part_width))
        rows = rows.reshape(slots, part_width)
        low, high = slice(0, slots // 2), slice(slots // 2, slots)
        forward, backward, on, back, own = partials(rows, *gate_ups)
        from_before = turned(forward, 1)
        from_after = turned(backward, -1)
        relay_on = (on + from_before[low].astype(jnp.float32)).astype(jnp.bfloat16)
        relay_back = (back + from_after[low].astype(jnp.float32)).astype(jnp.bfloat16)
        last_low = turned(relay_on, 1)
        last_high = turned(relay_back, -1)
        gate_up = jnp.concatenate(
            [
                own[low] + from_after[high].astype(jnp.float32) + last_low.astype(jnp.float32),
                own[high] + from_before[high].astype(jnp.float32) + last_high.astype(jnp.float32),
            ],
            axis=0,
        )
        gate, upper = jnp.split(gate_up, 2, axis=1)
        hidden = (jax.nn.silu(gate) * upper).astype(jnp.bfloat16)
        hiddens = [hidden] + [turned(hidden, by) for by in others]
        spread = dot(lax.optimization_barrier(jnp.concatenate(hiddens, axis=1)), downs)
        spread = spread.astype(jnp.bfloat16)
        returned = spread_out(spread.reshape(experts, -1, part_width))
        if finals:
            *finals[0], returned = lax.optimization_barrier((*finals[0], returned))
        returned = returned.reshape(slots, part_width)
        places = [wanted[:, k, None] == slot_ids[None, :] for k in range(choose)]
        combine = sum(jnp.where(p, weights[:, k, None], 0.0) for k, p in enumerate(places))
        shares = dot(jnp.concatenate(three_parts(combine), axis=0), returned)
        moe = jnp.sum(shares.reshape(3, half, part_width), axis=0)
        result = (mixed[h * half : (h + 1) * half] + moe).astype(jnp.bfloat16)
        blocks = half // sub
        finals.append(
            [piece(result, jnp.clip(me - h * blocks, 0, blocks - 1), sub, 0)]
            + [handed(result, by, h * blocks, blocks, sub) for by in others]
        )
    mine = [jnp.where(me * sub < half, a, b) for a, b in zip(*finals)]
    columns = in_order(mine, sources)
    return jnp.concatenate(columns, axis=1)


def solution(mesh):
    in_specs = (
        P("sp", None),
        P("sp", "tp"),
        P("tp", None, None),
        P("tp"),
        P("tp", None),
        P(),
        P("sp", None, "tp"),
        P("sp", None, "tp"),
        P("sp", "tp", None),
        P("sp", None),
        P("sp", None),
    )
    out_specs = P(("sp", "tp"), None)
    return jax.shard_map(
        on_device, mesh=mesh, in_specs=in_specs, out_specs=out_specs, check_vma=False
    )
```
